256 devices in a mesh: grp: 2 (over y), fs: 16 (over z), tp: 8 (over x, core).
Axes of the slice: x: 4, y: 2, z: 16, core: 2. Of those that a mesh axis runs over, the one named last changes fastest.
The devices are a block of a 4x16x16 slice.
Arguments:
- tokens: bfloat16 [32768, 2048], P(('grp', 'fs')), parts along dimension 0, may hold values from -1300 to 1300
- norm_gain: bfloat16 [2048], replicated, may hold values from 0.099609375 to 1.8984375
- gate_weight: bfloat16 [2048, 5120], P('fs', 'tp'), may hold values from -0.125 to 0.125
- up_weight: bfloat16 [2048, 5120], P('fs', 'tp'), may hold values from -0.125 to 0.125
- down_weight: bfloat16 [5120, 2048], P('tp', 'fs'), may hold values from -0.078125 to 0.078125
Outputs:
- mixed: bfloat16 [32768, 2048], P(('grp', 'fs', 'tp')), parts along dimension 0
The draws below stay inside these ranges and needn't reach their ends.
There are 2 independent parts, one for each index of `grp`. The reference program is written for one: setup_inputs(seed, part) draws one part's arguments, and reference() takes and returns one part's arrays. A program takes and returns all parts, laid end to end along the dimension named above; an argument that names none is the same for every part. Nothing has to cross between parts.
All inputs are finite; a program needn't handle non-finite values.
Results may differ from the reference program's by a relative error of at most 0.013.
Values may be sent and summed in bfloat16 or wider, within the bound.
No kernel may reach another device: no remote copies, remote signals or barrier semaphores. Data moves between devices by JAX's collectives and lax.ppermute only.
A program may use at most 64 MiB of HBM per device.

```python
import math
import jax
import jax.numpy as jnp
from jax import lax

D = 2048
FF = 5120
TOKENS = 16384
N_TP = 8


def draw_tokens(key, part):
    key_base = jax.random.fold_in(key, 11)
    key_rows = jax.random.fold_in(key, 12)
    key_cols = jax.random.fold_in(key, 13)
    col_scale = jnp.exp(jax.random.uniform(key_cols, (1, D), jnp.float32, 0.0, math.log(10.0)))
    base = jnp.clip(jax.random.normal(key_base, (TOKENS, D), jnp.float32), -5.0, 5.0)
    row_scale = jnp.exp(jax.random.uniform(key_rows, (TOKENS, 1), jnp.float32, 0.0, math.log(10.0)))
    return (base * row_scale * col_scale).astype(jnp.bfloat16)


def level_of(own_key, extent, cuts, least, high):
    def one(dim, shards_of):
        heights = jax.random.uniform(jax.random.fold_in(jax.random.fold_in(own_key, 6), dim), (shards_of,), jnp.float32, least / len(cuts), high / len(cuts))
        return jnp.repeat(jnp.exp(heights), extent[dim] // shards_of).reshape((-1,) + (1,) * (len(extent) - dim - 1))

    factor_of = one(*cuts[0])
    for cut in cuts[1:]:
        factor_of = factor_of * one(*cut)
    return factor_of


def noise(rng, shape, deviation, reach, pieces=(), dtype=jnp.bfloat16):
    result = deviation * jax.random.normal(rng, shape, jnp.float32)
    if pieces:
        result = result * level_of(rng, shape, pieces, -0.22, 0.18)
    return jnp.clip(result, -reach, reach).astype(dtype)


def setup_inputs(seed: int = 0, part: int = 0) -> dict:
    key_list = jax.random.split(jax.random.key(seed), 6)
    part_keys = jax.random.split(jax.random.fold_in(key_list[5], part), 6)
    return {
        "tokens": draw_tokens(jax.random.fold_in(jax.random.fold_in(key_list[5], part), 71), part),
        "norm_gain": jnp.clip(1.0 + 0.18 * jax.random.normal(key_list[1], (D,), jnp.float32), 0.099609375, 1.8984375).astype(jnp.bfloat16),
        "gate_weight": noise(key_list[2], (D, FF), D ** -0.5, 0.125, ((0, 16), (1, 8))),
        "up_weight": noise(key_list[3], (D, FF), D ** -0.5, 0.125, ((0, 16), (1, 8))),
        "down_weight": noise(key_list[4], (FF, D), FF ** -0.5, 0.078125, ((0, 8), (1, 16))),
    }


EPSILON = 1e-06

def reference(tokens, norm_gain, gate_weight, up_weight, down_weight):
    as_float = tokens.astype(jnp.float32)
    scale = lax.rsqrt(lax.optimization_barrier(jnp.mean(as_float * as_float, axis=-1, keepdims=True)) + EPSILON)
    normed = (as_float * scale * norm_gain.astype(jnp.float32)).astype(jnp.bfloat16)
    gate_acts = jnp.dot(normed, gate_weight, preferred_element_type=jnp.float32)
    up_acts = jnp.dot(normed, up_weight, preferred_element_type=jnp.float32)
    hidden = (jax.nn.silu(gate_acts) * up_acts).astype(jnp.bfloat16)
    group_width = FF // N_TP
    hidden_groups = jnp.transpose(hidden.reshape(TOKENS, N_TP, group_width), (1, 0, 2))
    down_groups = down_weight.reshape(N_TP, group_width, D)

    def accumulate(running, pair):
        hidden_part, weight_part = pair
        product = jnp.dot(hidden_part, weight_part, preferred_element_type=jnp.float32)
        partials = lax.optimization_barrier(product.astype(jnp.bfloat16)).astype(jnp.float32)
        return (running + partials, None)
    running, _ = lax.scan(accumulate, jnp.zeros((TOKENS, D), jnp.float32), (hidden_groups, down_groups))
    return running.astype(jnp.bfloat16)
```

```python
import functools

import jax
import jax.numpy as jnp
from jax import lax
from jax.experimental import pallas as pl
from jax.experimental.pallas import tpu as pltpu
from jax.sharding import PartitionSpec as P


EPSILON = 1e-06
B = 128
F32 = jnp.float32
BF16 = jnp.bfloat16


def hbm(v):
    return pltpu.with_memory_space_constraint(v, pltpu.HBM)


def vmem(mb):
    return pltpu.CompilerParams(vmem_limit_bytes=mb * 1024 * 1024)


def on_chip(n):
    return [pl.BlockSpec(memory_space=pltpu.VMEM)] * n


RING_BLOCKS = (("g", 0), ("g", 1), ("u", 0), ("u", 1), ("d", 0), ("g", 2), ("u", 2), ("d", 1), ("d", 2), ("d", 3))
PAIR_BLOCKS = (("g", 4), ("g", 3), ("u", 4), ("u", 3), ("d", 4))
SHARED = 5
SLOTS = 5


def pack(meta, gate, up, down):
    def body(m, g, u, d, zo, yo):
        def put(flip):
            for out, names in ((zo, RING_BLOCKS), (yo, PAIR_BLOCKS)):
                for n, (what, k) in enumerate(names):
                    c = slice((SLOTS - 1 - k if flip else k) * B, (SLOTS - k if flip else k + 1) * B)
                    out[n] = d[c, :] if what == "d" else (g if what == "g" else u)[:, c]

        pl.when(m[3] == 0)(lambda: put(False))
        pl.when(m[3] != 0)(lambda: put(True))

    whole = lambda v: pl.BlockSpec(v.shape, lambda i, m: (0, 0))
    return pl.pallas_call(
        body,
        grid_spec=pltpu.PrefetchScalarGridSpec(
            num_scalar_prefetch=1, grid=(1,), in_specs=[whole(gate), whole(up), whole(down)], out_specs=on_chip(2)
        ),
        out_shape=[pltpu.VMEM((len(RING_BLOCKS), B, B), gate.dtype), pltpu.VMEM((len(PAIR_BLOCKS), B, B), gate.dtype)],
        compiler_params=vmem(4),
    )(meta, hbm(gate), hbm(up), hbm(down))


def normalize(tokens, gain, meta, ring):
    rows, width = tokens.shape
    tile, step = 256, 16

    def body(m, t, g, out):
        z = m[2]

        def chunk(n, _):
            x = t[pl.ds(pl.multiple_of(n * step, step), step), :].astype(F32)
            scale = lax.rsqrt(jnp.mean(x * x, axis=-1, keepdims=True) + EPSILON)
            y = (x * scale * g[...].astype(F32)).astype(BF16)
            at = pl.ds(pl.multiple_of(pl.program_id(0) * tile + n * step, step), step)
            for b in range(ring):
                i = lax.rem(b - z + ring + ring // 2, ring)
                out[at, pl.ds(pl.multiple_of(i * B, B), B)] = y[:, b * B:(b + 1) * B]
            return 0

        lax.fori_loop(0, tile // step, chunk, 0, unroll=2)

    return pl.pallas_call(
        body,
        grid_spec=pltpu.PrefetchScalarGridSpec(
            num_scalar_prefetch=1,
            grid=(rows // tile,),
            in_specs=[pl.BlockSpec((tile, width), lambda i, m: (i, 0)), pl.BlockSpec((1, width), lambda i, m: (0, 0))],
            out_specs=on_chip(1)[0],
        ),
        out_shape=pltpu.VMEM((rows, width), BF16),
        compiler_params=vmem(8),
        cost_estimate=pl.CostEstimate(flops=rows * width * 16, bytes_accessed=rows * width * 4, transcendentals=0),
    )(meta, hbm(tokens), gain.reshape(1, width))


class Parts:
    def __init__(self, pieces, ids):
        self.args, self.where = [], {}
        for i in ids:
            for array, lo, names in pieces[i]:
                n = next((n for n, v in enumerate(self.args) if v is array), len(self.args))
                if n == len(self.args):
                    self.args.append(array)
                for j, name in enumerate(names):
                    self.where[i, name] = (n, lo + j)

    def block(self, refs, i, name):
        n, j = self.where[i, name]
        return refs[n][j]

    def gate_up(self, refs, ids, k):
        rows = [jnp.concatenate([self.block(refs, i, ("g", k)), self.block(refs, i, ("u", k))], axis=1) for i in ids]
        return jnp.concatenate(rows, axis=0)

    def down(self, refs, ids):
        cols = [jnp.concatenate([self.block(refs, i, ("d", k)) for k in range(SLOTS)], axis=0) for i in ids]
        return jnp.concatenate(cols, axis=1)


def runs(ids):
    out = []
    for i in ids:
        if out and out[-1][1] == i:
            out[-1][1] = i + 1
        else:
            out.append([i, i + 1])
    return out


def take(ref, rows, ids):
    cols = [ref[rows, a * B:b * B] for a, b in runs(ids)]
    return cols[0] if len(cols) == 1 else jnp.concatenate(cols, axis=1)


def accumulate(normed, ids, pieces, acc):
    rows = normed.shape[0]
    tile = 512
    gu = Parts(pieces, ids)
    old = [] if acc is None else [acc]

    def body(x, *rest):
        refs, out = rest[len(old):-1], rest[-1]
        for k in range(SLOTS):
            w = gu.gate_up(refs, ids, k)
            c = slice(2 * k * B, 2 * (k + 1) * B)
            for r in range(0, rows, tile):
                at = slice(r, r + tile)
                part = jnp.dot(take(x, at, ids), w, preferred_element_type=F32)
                out[at, c] = rest[0][at, c] + part if old else part

    return pl.pallas_call(
        body,
        in_specs=on_chip(1 + len(old) + len(gu.args)),
        out_specs=on_chip(1)[0],
        out_shape=pltpu.VMEM((rows, 2 * SLOTS * B), F32),
        input_output_aliases={1: 0} if old else {},
        compiler_params=vmem(6),
        cost_estimate=pl.CostEstimate(flops=4 * rows * len(ids) * B * SLOTS * B, bytes_accessed=rows * SLOTS * B * 16, transcendentals=0),
    )(normed, *old, *gu.args)


def finish(meta, normed, ids, pieces, acc, rel):
    rows = normed.shape[0]
    chips = rows // (2 * B)
    ring = len(pieces)
    parts = Parts(pieces, range(ring))

    def body(m, x, a, *rest):
        refs, (keep, send) = rest[:-2], rest[-2:]
        chip = lax.rem(m[0] + rel, chips)
        mine = pl.ds(pl.multiple_of((2 * chip + m[1]) * B, B), B)
        theirs = pl.ds(pl.multiple_of((2 * chip + 1 - m[1]) * B, B), B)
        v = jnp.concatenate([take(x, mine, ids), take(x, theirs, ids)], axis=0)
        h = []
        for k in range(SLOTS):
            c = slice(2 * k * B, 2 * (k + 1) * B)
            act = jnp.concatenate([a[mine, c], a[theirs, c]], axis=0)
            act = act + jnp.dot(v, parts.gate_up(refs, ids, k), preferred_element_type=F32)
            gate = act[:, :B]
            h.append((gate / (1.0 + jnp.exp(-gate)) * act[:, B:]).astype(BF16))
        h = jnp.concatenate(h, axis=1)
        for j in range(0, ring, 2):
            c = slice(j * B, (j + 2) * B)
            y = jnp.dot(h, parts.down(refs, [j, j + 1]), preferred_element_type=F32).astype(BF16)
            keep[:, c] = y[:B]
            send[:, c] = y[B:]

    half = pltpu.VMEM((B, ring * B), BF16)
    return pl.pallas_call(
        body,
        in_specs=[pl.BlockSpec(memory_space=pltpu.SMEM)] + on_chip(2 + len(parts.args)),
        out_specs=on_chip(2),
        out_shape=[half, half],
        compiler_params=vmem(6),
        cost_estimate=pl.CostEstimate(flops=4 * B * SLOTS * B * (2 * len(ids) * B + ring * B), bytes_accessed=8 << 20, transcendentals=2 * B * SLOTS * B),
    )(meta, normed, acc, *parts.args)


def both(a, b):
    return a[...].astype(F32) + b[...].astype(F32)


def far(keep, got):
    rows, cols = keep.shape
    h = rows // 2

    def body(k, g, a, b):
        v = both(k, g).astype(BF16)
        a[...] = v[:h]
        b[...] = v[h:]

    out = jax.ShapeDtypeStruct((h, cols), BF16)
    return pl.pallas_call(body, out_shape=[out, out], compiler_params=vmem(8))(keep, got)


def near(keep1, got1, keep3, got3, more):
    rows, cols = keep1.shape
    h = rows // 2

    def body(k1, g1, k3, g3, *rest):
        o1, o3 = rest[-2:]
        if more:
            o1[...] = (both(k1, g1) + rest[0][...].astype(F32)).astype(BF16)
            o3[...] = (both(k3, g3) + rest[1][...].astype(F32)).astype(BF16)
        else:
            o1[...] = both(k1, g1).astype(BF16)
            o3[...] = both(k3, g3).astype(BF16)

    top = pl.BlockSpec((h, cols), lambda i: (0, 0))
    low = pl.BlockSpec((h, cols), lambda i: (1, 0))
    first = [top, top, low, low] if more else [low, low, top, top]
    out = jax.ShapeDtypeStruct((h, cols), BF16)
    return pl.pallas_call(
        body, grid=(1,), in_specs=first + [top] * len(more), out_specs=[top, top], out_shape=[out, out], compiler_params=vmem(8)
    )(keep1, got1, keep3, got3, *more)


def total(meta, keep, got, free1, rest1, free3, rest3, ring):
    rows, cols = keep.shape
    h = rows // 2

    def body(m, k, g, f1, r1, f3, r3, out):
        top = (both(k.at[:h], g.at[:h]) + both(r1, f3)).astype(BF16)
        low = (both(k.at[h:], g.at[h:]) + both(f1, r3)).astype(BF16)
        for j in range(ring):
            at = pl.ds(pl.multiple_of(lax.rem(j + m[2] + ring // 2, ring) * B, B), B)
            out[:h, at] = top[:, j * B:(j + 1) * B]
            out[h:, at] = low[:, j * B:(j + 1) * B]

    full = pl.BlockSpec((rows, cols), lambda i, m: (0, 0))
    part = pl.BlockSpec((h, cols), lambda i, m: (0, 0))
    return pl.pallas_call(
        body,
        grid_spec=pltpu.PrefetchScalarGridSpec(num_scalar_prefetch=1, grid=(1,), in_specs=[full, full, part, part, part, part], out_specs=full),
        out_shape=jax.ShapeDtypeStruct((rows, cols), BF16),
        compiler_params=vmem(8),
    )(meta, keep, got, free1, rest1, free3, rest3)


def on_device(sizes, tokens, norm_gain, gate_weight, up_weight, down_weight):
    ring, tp, groups = sizes["fs"], sizes["tp"], sizes["grp"]
    half = ring // 2

    def shift(v, k):
        return lax.ppermute(v, "fs", [(i, (i + k) % ring) for i in range(ring)])

    def chip(v, k):
        return lax.ppermute(v, "tp", [(i, (i + 2 * k) % tp) for i in range(tp)])

    def core(v):
        return lax.ppermute(v, "tp", [(i, i ^ 1) for i in range(tp)])

    def pair(v):
        return lax.ppermute(v, "grp", [(i, i ^ 1) for i in range(groups)])

    t = lax.axis_index("tp")
    meta = jnp.stack([t // 2, t % 2, lax.axis_index("fs"), lax.axis_index("grp") % 2]).astype(jnp.int32)

    f, own = pack(meta, gate_weight, up_weight, down_weight)
    pieces = {half: [(f, 0, RING_BLOCKS), (own, 0, PAIR_BLOCKS)]}
    g = f
    for s in range(1, half):
        f = shift(f, 1)
        g = shift(g, -1)
        y = jnp.concatenate([f[:SHARED], g[:SHARED]])
        y = pair(y)
        pieces[half - s] = [(f, 0, RING_BLOCKS), (y, 0, PAIR_BLOCKS)]
        pieces[half + s] = [(g, 0, RING_BLOCKS), (y, SHARED, PAIR_BLOCKS)]
    f = shift(f[:SHARED], 1)
    g = shift(g[SHARED:], -1)
    y = pair(f)
    pieces[0] = [(f, 0, RING_BLOCKS[:SHARED]), (g, 0, RING_BLOCKS[SHARED:]), (y, 0, PAIR_BLOCKS)]
    normed = normalize(tokens, norm_gain, meta, ring)
    acc = accumulate(normed, list(range(half - 3, half + 4)), pieces, None)
    acc = accumulate(normed, [2, 3, 4, ring - 4, ring - 3, ring - 2], pieces, acc)
    last = [0, 1, ring - 1]
    done = {}
    for rel in (2, 1, 3, 0):
        keep, send = finish(meta, normed, last, pieces, acc, rel)
        done[rel] = (keep, core(send))
    a, b = far(*done[2])
    a, b = chip(a, 1), chip(b, -1)
    f1, f3 = near(*done[1], *done[3], ())
    f1, f3 = chip(f1, 1), chip(f3, -1)
    r1, r3 = near(*done[1], *done[3], (a, b))
    r1, r3 = chip(r1, 1), chip(r3, -1)
    return total(meta, *done[0], f1, r1, f3, r3, ring)


def solution(mesh):
    spec = P(("grp", "fs"), None)
    return jax.shard_map(
        functools.partial(on_device, dict(mesh.shape)),
        mesh=mesh,
        in_specs=(spec, P(), P("fs", "tp"), P("fs", "tp"), P("tp", "fs")),
        out_specs=P(("grp", "fs", "tp"), None),
        check_vma=False,
    )
```

```python
import functools

import jax
import jax.numpy as jnp
from jax import lax
from jax.experimental import pallas as pl
from jax.experimental.pallas import tpu as pltpu
from jax.sharding import PartitionSpec as P


EPSILON = 1e-06
B = 128
F32 = jnp.float32
BF16 = jnp.bfloat16


def hbm(v):
    return pltpu.with_memory_space_constraint(v, pltpu.HBM)


def vmem(mb):
    return pltpu.CompilerParams(vmem_limit_bytes=mb * 1024 * 1024)


def on_chip(n):
    return [pl.BlockSpec(memory_space=pltpu.VMEM)] * n


SLOTS = 5
SHARED = (("g", 0), ("g", 1), ("u", 0), ("u", 1), ("d", 0))
ALONE = (("g", 2), ("u", 2), ("d", 1), ("d", 2), ("d", 3))
PAIRED = tuple((what, SLOTS - 1 - k) for what, k in SHARED)


def other(names):
    return tuple((what, k + SLOTS) for what, k in names)


def own_first(names):
    return names + other(names)


def other_first(names):
    return other(names) + names


def pack(meta, gate, up, down):
    names = SHARED + ALONE + PAIRED

    def body(m, g, u, d, out):
        def put(flip):
            for n, (what, k) in enumerate(names):
                c = slice((SLOTS - 1 - k if flip else k) * B, (SLOTS - k if flip else k + 1) * B)
                out[n] = d[c, :] if what == "d" else (g if what == "g" else u)[:, c]

        pl.when(m[3] == 0)(lambda: put(False))
        pl.when(m[3] != 0)(lambda: put(True))

    whole = lambda v: pl.BlockSpec(v.shape, lambda i, m: (0, 0))
    return pl.pallas_call(
        body,
        grid_spec=pltpu.PrefetchScalarGridSpec(
            num_scalar_prefetch=1, grid=(1,), in_specs=[whole(gate), whole(up), whole(down)], out_specs=on_chip(1)[0]
        ),
        out_shape=pltpu.VMEM((len(names), B, B), gate.dtype),
        compiler_params=vmem(4),
    )(meta, hbm(gate), hbm(up), hbm(down))


def place(m, i, ring):
    o = i - ring // 2
    return lax.rem(m[2] + jnp.where(m[1] == 0, o, -o) + 2 * ring, ring)


def normalize(tokens, gain, meta, ring):
    rows, width = tokens.shape
    chips = rows // (2 * B)

    def body(m, t, g, out):
        block = lambda b: t[:, b * B:(b + 1) * B].astype(F32)
        square = block(0) * block(0)
        for b in range(1, ring):
            square = square + block(b) * block(b)
        scale = lax.rsqrt(jnp.sum(square, axis=-1, keepdims=True) * (1.0 / width) + EPSILON)
        at = pl.ds(pl.multiple_of(pl.program_id(0) * B, B), B)
        for b in range(ring):
            d = b - m[2] + ring
            i = lax.rem(jnp.where(m[1] == 0, d, 2 * ring - d) + ring // 2, ring)
            y = block(b) * scale * g[:, b * B:(b + 1) * B].astype(F32)
            out[at, pl.ds(pl.multiple_of(i * B, B), B)] = y.astype(BF16)

    return pl.pallas_call(
        body,
        grid_spec=pltpu.PrefetchScalarGridSpec(
            num_scalar_prefetch=1,
            grid=(chips,),
            in_specs=[pl.BlockSpec((B, width), lambda i, m: (2 * lax.rem(m[0] + i, chips) + m[1], 0)), pl.BlockSpec((1, width), lambda i, m: (0, 0))],
            out_specs=on_chip(1)[0],
        ),
        out_shape=pltpu.VMEM((chips * B, width), BF16),
        compiler_params=vmem(8),
        cost_estimate=pl.CostEstimate(flops=rows * width * 8, bytes_accessed=rows * width * 2, transcendentals=0),
    )(meta, hbm(tokens), gain.reshape(1, width))


class Parts:
    def __init__(self, pieces, ids):
        self.args, self.where = [], {}
        for i in ids:
            for array, lo, names in pieces[i]:
                n = next((n for n, v in enumerate(self.args) if v is array), len(self.args))
                if n == len(self.args):
                    self.args.append(array)
                for j, name in enumerate(names):
                    self.where[i, name] = (n, lo + j)

    def block(self, refs, i, name):
        n, j = self.where[i, name]
        return refs[n][j]

    def gate_up(self, refs, ids, k):
        rows = [jnp.concatenate([self.block(refs, i, ("g", k)), self.block(refs, i, ("u", k))], axis=1) for i in ids]
        return jnp.concatenate(rows, axis=0)

    def down(self, refs, ids):
        cols = [jnp.concatenate([self.block(refs, i, ("d", k)) for k in range(2 * SLOTS)], axis=0) for i in ids]
        return jnp.concatenate(cols, axis=1)


def runs(ids):
    out = []
    for i in ids:
        if out and out[-1][1] == i:
            out[-1][1] = i + 1
        else:
            out.append([i, i + 1])
    return out


def take(ref, rows, ids):
    cols = [ref[rows, a * B:b * B] for a, b in runs(ids)]
    return cols[0] if len(cols) == 1 else jnp.concatenate(cols, axis=1)


def accumulate(normed, ids, pieces, acc):
    rows = normed.shape[0]
    gu = Parts(pieces, ids)
    old = [] if acc is None else [acc]

    def body(x, *rest):
        refs, out = rest[len(old):-1], rest[-1]
        v = take(x, slice(0, rows), ids)
        for k in range(2 * SLOTS):
            c = slice(2 * k * B, 2 * (k + 1) * B)
            part = jnp.dot(v, gu.gate_up(refs, ids, k), preferred_element_type=F32)
            out[:, c] = rest[0][:, c] + part if old else part

    return pl.pallas_call(
        body,
        in_specs=on_chip(1 + len(old) + len(gu.args)),
        out_specs=on_chip(1)[0],
        out_shape=pltpu.VMEM((rows, 4 * SLOTS * B), F32),
        input_output_aliases={1: 0} if old else {},
        compiler_params=vmem(6),
        cost_estimate=pl.CostEstimate(flops=8 * rows * len(ids) * B * SLOTS * B, bytes_accessed=rows * SLOTS * B * 32, transcendentals=0),
    )(normed, *old, *gu.args)


def finish(normed, ids, pieces, acc, rels, outs):
    ring = len(pieces)
    parts = Parts(pieces, range(ring))
    many = len(rels) * B

    def body(x, a, *rest):
        refs, out = rest[:len(parts.args)], rest[len(parts.args):]
        row = [slice(r * B, (r + 1) * B) for r in rels]
        v = jnp.concatenate([take(x, r, ids) for r in row], axis=0)
        h = []
        for k in range(2 * SLOTS):
            c = slice(2 * k * B, 2 * (k + 1) * B)
            act = jnp.concatenate([a[r, c] for r in row], axis=0)
            act = act + jnp.dot(v, parts.gate_up(refs, ids, k), preferred_element_type=F32)
            gate = act[:, :B]
            h.append((gate / (1.0 + jnp.exp(-gate)) * act[:, B:]).astype(BF16))
        h = jnp.concatenate(h, axis=1)
        for j in range(0, ring, 2):
            c = slice(j * B, (j + 2) * B)
            y = jnp.dot(h, parts.down(refs, [j, j + 1]), preferred_element_type=F32)
            for o, (rel, rows, kind) in zip(out, outs):
                lo = rels.index(rel) * B
                o[:, c] = y[lo + rows.start:lo + rows.stop].astype(kind)

    return pl.pallas_call(
        body,
        in_specs=on_chip(2 + len(parts.args)),
        out_specs=on_chip(len(outs)),
        out_shape=[pltpu.VMEM((rows.stop - rows.start, ring * B), kind) for _, rows, kind in outs],
        compiler_params=vmem(6),
        cost_estimate=pl.CostEstimate(flops=4 * many * SLOTS * B * (2 * len(ids) * B + ring * B), bytes_accessed=8 << 20, transcendentals=many * 2 * SLOTS * B),
    )(normed, acc, *parts.args)


def add(pairs):
    def body(*refs):
        n = len(pairs)
        for i in range(n):
            refs[2 * n + i][...] = (refs[2 * i][...] + refs[2 * i + 1][...].astype(F32)).astype(BF16)

    return pl.pallas_call(
        body, in_specs=on_chip(2 * len(pairs)), out_specs=on_chip(len(pairs)),
        out_shape=[pltpu.VMEM(p.shape, BF16) for p, _ in pairs], compiler_params=vmem(4),
    )(*[v for p in pairs for v in p])


def total(meta, keep, free1, rest1, free3, rest3, ring):
    rows, cols = keep.shape
    h = rows // 2

    def body(m, k, f1, r1, f3, r3, out):
        for j in range(ring):
            c = slice(j * B, (j + 1) * B)
            at = pl.ds(pl.multiple_of(place(m, j, ring) * B, B), B)
            out[:h, at] = (k[:h, c] + (r1[:, c].astype(F32) + f3[:, c].astype(F32))).astype(BF16)
            out[h:, at] = (k[h:, c] + (f1[:, c].astype(F32) + r3[:, c].astype(F32))).astype(BF16)

    return pl.pallas_call(
        body,
        in_specs=[pl.BlockSpec(memory_space=pltpu.SMEM)] + on_chip(5),
        out_specs=pl.BlockSpec((rows, cols), lambda: (0, 0)),
        out_shape=jax.ShapeDtypeStruct((rows, cols), BF16),
        compiler_params=vmem(4),
    )(meta, keep, free1, rest1, free3, rest3)


def on_device(sizes, tokens, norm_gain, gate_weight, up_weight, down_weight):
    ring, tp, groups = sizes["fs"], sizes["tp"], sizes["grp"]
    half = ring // 2

    def shift(v):
        way = [(i * tp + t, (i + 1 - 2 * (t % 2)) % ring * tp + t) for i in range(ring) for t in range(tp)]
        return lax.ppermute(v, ("fs", "tp"), way)

    def chip(v, k):
        return lax.ppermute(v, "tp", [(i, (i + 2 * k) % tp) for i in range(tp)])

    def core(v):
        return lax.ppermute(v, "tp", [(i, i ^ 1) for i in range(tp)])

    def pair(v):
        return lax.ppermute(v, "grp", [(i, i ^ 1) for i in range(groups)])

    def join(*parts):
        return jnp.concatenate(parts)

    t = lax.axis_index("tp")
    meta = jnp.stack([t // 2, t % 2, lax.axis_index("fs"), lax.axis_index("grp") % 2]).astype(jnp.int32)
    n = len(SHARED)

    own = pack(meta, gate_weight, up_weight, down_weight)
    theirs = core(own)
    every = SHARED + ALONE + PAIRED
    pieces = {half: [(own, 0, every), (theirs, 0, other(every))]}
    m = join(own[:n], theirs[:n])
    a = join(own[n:2 * n], theirs[n:2 * n])
    waiting = []

    def forward():
        d, at = core(join(*[v for v, _, _ in waiting])), 0
        for v, i, names in waiting:
            pieces[i].append((d, at, names))
            at += len(names)
        waiting.clear()

    for s in range(1, half):
        m = shift(m)
        a = shift(a)
        pieces[half - s] = [(m, 0, own_first(SHARED)), (a, 0, own_first(ALONE))]
        pieces[half + s] = []
        waiting += [(m, half + s, other_first(SHARED)), (a, half + s, other_first(ALONE))]
        if s > 1:
            forward()
        y = pair(m)
        pieces[half - s].append((y, 0, own_first(PAIRED)))
        waiting.append((y, half + s, other_first(PAIRED)))
    m = jnp.concatenate([m[:n], a[:n]])
    m = shift(m)
    pieces[0] = [(m, 0, SHARED + ALONE)]
    waiting.append((m, 0, other(SHARED + ALONE)))
    forward()
    y = pair(m[:n])
    pieces[0] += [(y, 0, PAIRED), (core(y), 0, other(PAIRED))]
    normed = normalize(tokens, norm_gain, meta, ring)
    acc = accumulate(normed, list(range(half - 3, half + 4)), pieces, None)
    acc = accumulate(normed, [2, 3, 4, ring - 4, ring - 3, ring - 2], pieces, acc)
    last = [0, 1, ring - 1]
    top, low = slice(0, B // 2), slice(B // 2, B)
    a, b = finish(normed, last, pieces, acc, [2], [(2, top, BF16), (2, low, BF16)])
    a, b = chip(a, 1), chip(b, -1)
    f1, w1, f3, w3 = finish(normed, last, pieces, acc, [1, 3], [(1, low, BF16), (1, top, F32), (3, top, BF16), (3, low, F32)])
    f1, f3 = chip(f1, 1), chip(f3, -1)
    (keep,) = finish(normed, last, pieces, acc, [0], [(0, slice(0, B), F32)])
    r1, r3 = add(((w1, a), (w3, b)))
    r1, r3 = chip(r1, 1), chip(r3, -1)
    return total(meta, keep, f1, r1, f3, r3, ring)


def solution(mesh):
    spec = P(("grp", "fs"), None)
    return jax.shard_map(
        functools.partial(on_device, dict(mesh.shape)),
        mesh=mesh,
        in_specs=(spec, P(), P("fs", "tp"), P("fs", "tp"), P("tp", "fs")),
        out_specs=P(("grp", "fs", "tp"), None),
        check_vma=False,
    )
```
